32 devices in a mesh: sp: 8 (over z, y), tp: 4 (over x, core).
Axes of the slice: x: 2, y: 2, z: 4, core: 2. Of those that a mesh axis runs over, the one named last changes fastest.
Arguments:
- tokens: bfloat16 [8192, 2048], P('sp'), may hold values from -6 to 6
- in_gain: float32 [2048], replicated, may hold values from 0.1 to 1.9
- w_query: bfloat16 [2048, 1024], P(None, 'tp'), may hold values from -0.125 to 0.125
- w_forget: bfloat16 [2048, 1024], P(None, 'tp'), may hold values from -0.125 to 0.125
- w_input: bfloat16 [2048, 1024], P(None, 'tp'), may hold values from -0.125 to 0.125
- w_outgate: bfloat16 [2048, 1024], P(None, 'tp'), may hold values from -0.125 to 0.125
- w_conv_h: bfloat16 [2048, 1024], P(None, 'tp'), may hold values from -0.125 to 0.125
- w_conv_b: bfloat16 [2048, 1024], P(None, 'tp'), may hold values from -0.125 to 0.125
- w_conv_c: bfloat16 [2048, 1024], P(None, 'tp'), may hold values from -0.125 to 0.125
- forget_floor: float32 [1024], P('tp'), may hold values from 0.84 to 1
- forget_leak: float32 [8192, 1024], P('sp', 'tp'), may hold values from -1 to 0
- state_gain: float32 [128], replicated, may hold values from 0.1 to 1.9
- conv_taps: bfloat16 [3, 1024], P(None, 'tp'), may hold values from -3.5 to 3.5
- group_gain: float32 [128], replicated, may hold values from 0.1 to 1.9
- out_state: bfloat16 [1024, 2048], P('tp'), may hold values from -0.1875 to 0.1875
- out_conv: bfloat16 [1024, 2048], P('tp'), may hold values from -0.1875 to 0.1875
Outputs:
- mixed_out: bfloat16 [8192, 2048], P('sp', 'tp')
The draws below stay inside these ranges and needn't reach their ends.
All inputs are finite; a program needn't handle non-finite values.
Results may differ from the reference program's by a relative error of at most 0.015.
Values may be sent and summed in bfloat16 or wider, within the bound.
A program may use at most 128 MiB of HBM per device.

```python
import jax
import jax.numpy as jnp
from jax import lax

D = 2048
GROUP_FEATURES = 128
MIXER_COUNT = 8
CONV_CH = 1024
BLOCK = 64
TAPS = 3
TOK_DEV = 1024
STEP_COUNT = 8192
STATE_W = 1024
MIX = 2048


def draw_forget_floor(key, part):
    key_fast, key_gap, key_slow = jax.random.split(jax.random.fold_in(key, 11), 3)
    share = 0.5
    is_fast = jax.random.uniform(key_fast, (MIXER_COUNT,)) < share
    is_fast = jnp.repeat(is_fast, GROUP_FEATURES)
    fast_gap = jnp.exp(jax.random.uniform(key_gap, (STATE_W,), jnp.float32, jnp.log(0.05), jnp.log(0.15)))
    slow_gap = jnp.exp(jax.random.uniform(key_slow, (STATE_W,), jnp.float32, jnp.log(0.2), jnp.log(1.0))) / STEP_COUNT
    return (1.0 - jnp.where(is_fast, fast_gap, slow_gap)).astype(jnp.float32)


def draw_forget_leak(key, part):
    key_scale, random_seed_site, key_depth, key_jitter = jax.random.split(jax.random.fold_in(key, 23), 4)
    nblk = STEP_COUNT // TOK_DEV
    low, high = (jnp.log(0.5), jnp.log(2.0))
    block_scale = jnp.exp(jax.random.uniform(key_scale, (nblk, MIXER_COUNT), jnp.float32, low, high))
    block_scale = jnp.repeat(jnp.repeat(block_scale, TOK_DEV, axis=0), GROUP_FEATURES, axis=1)
    jitter = jax.random.uniform(key_jitter, (STEP_COUNT, STATE_W), jnp.float32, 0.5, 1.5)
    starting_shift = -0.2 / STEP_COUNT * block_scale * jitter
    span_start = jax.random.randint(random_seed_site, (3, MIXER_COUNT), 0, STEP_COUNT)
    layer_number = jax.random.uniform(key_depth, (3, MIXER_COUNT), jnp.float32, jnp.log(0.5), jnp.log(0.8))
    element_places = jnp.arange(STEP_COUNT)[:, None]
    span_sizes = jnp.zeros((STEP_COUNT, MIXER_COUNT), jnp.float32)
    for entry_number in range(3):
        span_sizes = span_sizes + jnp.where(element_places == span_start[entry_number][None, :], layer_number[entry_number][None, :], 0.0)
    return (starting_shift + jnp.repeat(span_sizes, GROUP_FEATURES, axis=1)).astype(jnp.float32)


def with_spikes(values, key, source, target, parts, factor):
    owner, partner = [(jnp.arange(values.shape[position]) // (values.shape[position] // parts)).reshape([-1 if axis == position else 1 for axis in range(values.ndim)]) for position in (source, target)]
    chosen = jax.random.permutation(key, parts)[partner]
    strong = (owner == chosen) | (owner == (partner + parts // 2) % parts)
    return jnp.where(strong, factor * values, values)


def levels(key, dims, pieces, least, largest):
    level, own = 1.0, jax.random.fold_in(key, 6)
    for dim, parts in pieces:
        steps = jnp.exp(jax.random.uniform(jax.random.fold_in(own, dim), (parts,), jnp.float32, least / len(pieces), largest / len(pieces)))
        level = level * jnp.repeat(steps, dims[dim] // parts).reshape([-1 if axis == dim else 1 for axis in range(len(dims))])
    return level


def centred(rng, extent, spread, reach, cuts=(), held_as=jnp.bfloat16):
    loudness = levels(rng, extent, cuts, -0.22, 0.18) if cuts else 1.0
    array = jax.random.normal(rng, extent, jnp.float32) * spread * loudness
    return jnp.minimum(jnp.maximum(array, -reach), reach).astype(held_as)


def heavy_noise(own_key, dims, width, limit, shards, heavy, dtype=jnp.bfloat16):
    values = width * jax.random.normal(own_key, dims, jnp.float32)
    if shards:
        values = values * levels(own_key, dims, shards, -0.22, 0.18)
    return jnp.clip(with_spikes(values, jax.random.fold_in(own_key, 3), *heavy), -limit, limit).astype(dtype)


def setup_inputs(seed: int = 0) -> dict:
    streams_of = jax.random.split(jax.random.key(seed), 17)
    return {
        "tokens": centred(streams_of[0], (STEP_COUNT, D), 1.0, 6.0, ((0, 8),)),
        "in_gain": jnp.clip(1.0 + 0.18 * jax.random.normal(streams_of[1], (D,), jnp.float32), 0.1, 1.9),
        "w_query": centred(streams_of[2], (D, STATE_W), D ** -0.5, 0.125, ((1, 4),)),
        "w_forget": centred(streams_of[3], (D, STATE_W), D ** -0.5, 0.125, ((1, 4),)),
        "w_input": centred(streams_of[4], (D, STATE_W), D ** -0.5, 0.125, ((1, 4),)),
        "w_outgate": centred(streams_of[5], (D, STATE_W), D ** -0.5, 0.125, ((1, 4),)),
        "w_conv_h": centred(streams_of[6], (D, CONV_CH), D ** -0.5, 0.125, ((1, 4),)),
        "w_conv_b": centred(streams_of[7], (D, CONV_CH), D ** -0.5, 0.125, ((1, 4),)),
        "w_conv_c": centred(streams_of[8], (D, CONV_CH), D ** -0.5, 0.125, ((1, 4),)),
        "forget_floor": draw_forget_floor(jax.random.fold_in(streams_of[16], 71), 0),
        "forget_leak": draw_forget_leak(jax.random.fold_in(streams_of[16], 71), 0),
        "state_gain": jnp.clip(1.0 + 0.18 * jax.random.normal(streams_of[11], (GROUP_FEATURES,), jnp.float32), 0.1, 1.9),
        "conv_taps": centred(streams_of[12], (TAPS, CONV_CH), TAPS ** -0.5, 3.5, ((1, 4),)),
        "group_gain": jnp.clip(1.0 + 0.18 * jax.random.normal(streams_of[13], (GROUP_FEATURES,), jnp.float32), 0.1, 1.9),
        "out_state": heavy_noise(streams_of[14], (STATE_W, D), MIX ** -0.5, 0.1875, ((0, 4),), (0, 1, 4, 2.0)),
        "out_conv": heavy_noise(streams_of[15], (CONV_CH, D), MIX ** -0.5, 0.1875, ((0, 4),), (0, 1, 4, 2.0)),
    }


norm_eps = 1e-06
highest = lax.Precision.HIGHEST

def rms_rows(values, gain):
    scale = lax.rsqrt(lax.optimization_barrier(jnp.mean(values * values, axis=-1, keepdims=True)) + norm_eps)
    return values * scale * gain.astype(jnp.float32)

def state_block(carry_state, inputs):
    query_blk, key_blk, value_blk, logf_blk = inputs
    cum_log = jnp.cumsum(logf_blk, axis=1)
    carried = jnp.einsum('hcd,hde->hce', query_blk * jnp.exp(cum_log), carry_state, precision=highest)
    length = logf_blk.shape[1]
    causal = (jnp.arange(length)[:, None] >= jnp.arange(length)[None, :])[None, :, :, None]
    diff_log = cum_log[:, :, None, :] - cum_log[:, None, :, :]
    decay_all = jnp.exp(jnp.where(causal, diff_log, -jnp.inf))
    scores = jnp.einsum('hid,hjd,hijd->hij', query_blk, key_blk, decay_all, precision=highest)
    result = carried + jnp.einsum('hij,hje->hie', scores, value_blk, precision=highest)
    last_log = cum_log[:, -1, :]
    fresh = jnp.einsum('hcd,hce->hde', key_blk * jnp.exp(last_log[:, None, :] - cum_log), value_blk, precision=highest)
    new_state = jnp.exp(last_log)[:, :, None] * carry_state + fresh
    return (new_state, result)

def reference(tokens, in_gain, w_query, w_forget, w_input, w_outgate, w_conv_h, w_conv_b, w_conv_c, forget_floor, forget_leak, state_gain, conv_taps, group_gain, out_state, out_conv):
    count = tokens.shape[0]
    heads = MIXER_COUNT
    normed = rms_rows(tokens.astype(jnp.float32), in_gain).astype(jnp.bfloat16)

    def project(weight):
        return jnp.dot(normed, weight, preferred_element_type=jnp.float32).astype(jnp.bfloat16)
    proj_query = project(w_query)
    proj_forget = project(w_forget)
    proj_input = project(w_input)
    proj_outgate = project(w_outgate)
    proj_h = project(w_conv_h)
    proj_b = project(w_conv_b)
    proj_c = project(w_conv_c)
    gate_logit = proj_forget.astype(jnp.float32)
    log_forget = jnp.logaddexp(jnp.log(forget_floor), jnp.log1p(-forget_floor) + jax.nn.log_sigmoid(gate_logit)) + forget_leak
    key_gate = (1.0 - forget_floor) * jax.nn.sigmoid(-gate_logit)
    query_act = jax.nn.silu(proj_query.astype(jnp.float32))
    value_f = proj_input.astype(jnp.float32)
    nblk = count // BLOCK

    def to_blocks(arr):
        return arr.reshape(nblk, BLOCK, heads, GROUP_FEATURES).transpose(0, 2, 1, 3)
    start_state = jnp.zeros((heads, GROUP_FEATURES, GROUP_FEATURES), jnp.float32)
    _, outputs = lax.scan(state_block, start_state, (to_blocks(query_act), to_blocks(key_gate), to_blocks(value_f), to_blocks(log_forget)))
    state_read = outputs.transpose(0, 2, 1, 3).reshape(count, heads, GROUP_FEATURES)
    out_gate = jax.nn.silu(proj_outgate.astype(jnp.float32)).reshape(count, heads, GROUP_FEATURES)
    state_res = (rms_rows(state_read, state_gain) * out_gate).reshape(count, STATE_W).astype(jnp.bfloat16)
    conv_in = (proj_c.astype(jnp.float32) * proj_h.astype(jnp.float32)).astype(jnp.bfloat16)
    padded = jnp.concatenate([jnp.zeros((TAPS - 1, CONV_CH), jnp.bfloat16), conv_in], axis=0).astype(jnp.float32)
    taps_f = conv_taps.astype(jnp.float32)
    conv_sum = jnp.zeros((count, CONV_CH), jnp.float32)
    for offset in range(TAPS):
        conv_sum = conv_sum + taps_f[offset][None, :] * padded[offset:offset + count]
    gated = (proj_b.astype(jnp.float32) * conv_sum).reshape(count, CONV_CH // GROUP_FEATURES, GROUP_FEATURES)
    conv_res = rms_rows(gated, group_gain).reshape(count, CONV_CH).astype(jnp.bfloat16)
    total = jnp.dot(state_res, out_state, preferred_element_type=jnp.float32)
    total = total + jnp.dot(conv_res, out_conv, preferred_element_type=jnp.float32)
    return total.astype(jnp.bfloat16)
```

```python
import functools

import jax
import jax.numpy as jnp
from jax import lax
from jax.experimental import pallas as pl
from jax.experimental.pallas import tpu as pltpu
from jax.sharding import PartitionSpec as P

GROUP_FEATURES = 128
CHUNK = 128
ROWS = 256
TAPS = 3
HALO = 8

norm_eps = 1e-06
f32 = jnp.float32
bf16 = jnp.bfloat16


def dot(a, b, dims=((1,), (0,)), precision=None):
    return lax.dot_general(a, b, (dims, ((), ())), precision=precision, preferred_element_type=f32)


def rms(values):
    return values * lax.rsqrt(jnp.mean(values * values, axis=-1, keepdims=True) + norm_eps)


def per_group(values, gain):
    parts = []
    for g in range(values.shape[1] // GROUP_FEATURES):
        parts.append(rms(values[:, g * GROUP_FEATURES : (g + 1) * GROUP_FEATURES]) * gain)
    return jnp.concatenate(parts, axis=1)


def local_kernel(
    tokens, in_gain, wq, wf, wi, wg, wh, wb, wc, floor, leak, taps, group_gain,
    read_out, qdev_out, gate_out, conv_out, state_out, log_out, conv_tail, head_conv, head_gate,
    pad, state, offset,
):
    step = pl.program_id(0)
    rows = tokens.shape[0]

    @pl.when(step == 0)
    def _():
        pad[0:HALO, :] = jnp.zeros((HALO, pad.shape[1]), f32)
        state[...] = jnp.zeros_like(state)
        offset[...] = jnp.zeros_like(offset)

    normed = (rms(tokens[...].astype(f32)) * in_gain[...]).astype(bf16)

    def project(w):
        return dot(normed, w[...]).astype(bf16).astype(f32)

    conv_in = (project(wc) * project(wh)).astype(bf16).astype(f32)
    proj_b = project(wb)
    pad[HALO : HALO + rows, :] = conv_in
    t = taps[...].astype(f32)
    total = t[TAPS - 1 : TAPS] * conv_in
    for j in range(TAPS - 1):
        total += t[j : j + 1] * pad[HALO - (TAPS - 1) + j : HALO - (TAPS - 1) + j + rows, :]
    conv_out[...] = per_group(proj_b * total, group_gain[...]).astype(bf16)

    @pl.when(step == 0)
    def _():
        head_conv[...] = conv_in[:HALO].astype(bf16)
        head_gate[...] = proj_b[:HALO].astype(bf16)

    tail = conv_in[rows - HALO :]
    pad[0:HALO, :] = tail
    conv_tail[...] = tail.astype(bf16)

    x = project(wf)
    key = (1.0 - floor[...]) * jax.nn.sigmoid(-x)
    logf = jnp.log(1.0 - key) + leak[...]
    value = dot(normed, wi[...]).astype(bf16)
    query = jax.nn.silu(project(wq))
    gate_out[...] = dot(normed, wg[...]).astype(bf16)

    r = lax.broadcasted_iota(jnp.int32, (CHUNK, CHUNK), 0)
    c = lax.broadcasted_iota(jnp.int32, (CHUNK, CHUNK), 1)
    causal = r >= c
    ones = causal.astype(f32)
    for b in range(rows // CHUNK):
        lo, hi = b * CHUNK, (b + 1) * CHUNK
        cum = dot(ones, logf[lo:hi], precision=lax.Precision.HIGHEST)
        mid = cum[CHUNK // 2 - 1 : CHUNK // 2]
        last = cum[CHUNK - 1 : CHUNK]
        q_mid = query[lo:hi] * jnp.exp(cum - mid)
        k_mid = key[lo:hi] * jnp.exp(mid - cum)
        q_all = q_mid * jnp.exp(mid)
        k_end = (k_mid * jnp.exp(last - mid)).astype(bf16)
        qdev_out[lo:hi, :] = (q_all * jnp.exp(offset[...])).astype(bf16)
        q_mid, k_mid, q_all = q_mid.astype(bf16), k_mid.astype(bf16), q_all.astype(bf16)
        for h in range(value.shape[1] // GROUP_FEATURES):
            s = slice(h * GROUP_FEATURES, (h + 1) * GROUP_FEATURES)
            scores = dot(q_mid[:, s], k_mid[:, s], ((1,), (1,)))
            scores = jnp.where(causal, scores, 0.0).astype(bf16)
            v = value[lo:hi, s]
            held = state[h]
            read_out[lo:hi, s] = dot(scores, v) + dot(q_all[:, s], held.astype(bf16), ((1,), (1,)))
            state[h] = held * jnp.exp(last[:, s]) + dot(v, k_end[:, s], ((0,), (0,)))
        offset[...] += last
    state_out[...] = state[...].astype(bf16)
    log_out[...] = offset[...]


def merge_kernel(
    read, qdev, gate, conv, states, logs, rim, head_conv, head_gate, state_gain, group_gain, taps,
    mixed, incoming,
):
    place = lax.axis_index("sp")
    heads, rows = states.shape[1], read.shape[0]

    @pl.when(pl.program_id(0) == 0)
    def _():
        incoming[...] = jnp.zeros_like(incoming)

        def hop(p, _):
            decay = jnp.exp(logs[pl.ds(p, 1)][0])
            for h in range(heads):
                s = slice(h * GROUP_FEATURES, (h + 1) * GROUP_FEATURES)
                incoming[h] = incoming[h] * decay[:, s] + states[pl.ds(p, 1)][0, h].astype(f32)
            return 0

        lax.fori_loop(0, place, hop, 0)

    width = heads * GROUP_FEATURES
    for h in range(heads):
        s = slice(h * GROUP_FEATURES, (h + 1) * GROUP_FEATURES)
        whole = read[:, s] + dot(qdev[:, s], incoming[h].astype(bf16), ((1,), (1,)))
        out = rms(whole) * state_gain[...] * jax.nn.silu(gate[:, s].astype(f32))
        mixed[:, s] = out.astype(bf16)
    mixed[:, width:] = conv[...]

    @pl.when(pl.program_id(0) == 0)
    def _():
        t = taps[...].astype(f32)
        own = head_conv[...].astype(f32)
        ext = jnp.concatenate([rim[...].astype(f32), own], axis=0)
        total = t[TAPS - 1 : TAPS] * own
        for j in range(TAPS - 1):
            total += t[j : j + 1] * ext[HALO - (TAPS - 1) + j : 2 * HALO - (TAPS - 1) + j]
        fixed = per_group(head_gate[...].astype(f32) * total, group_gain[...])
        mixed[0:HALO, width:] = fixed.astype(bf16)


def body(
    tokens, in_gain, w_query, w_forget, w_input, w_outgate, w_conv_h, w_conv_b, w_conv_c,
    forget_floor, forget_leak, state_gain, conv_taps, group_gain, out_state, out_conv,
):
    count, feats = tokens.shape
    width, channels = w_query.shape[1], w_conv_h.shape[1]
    heads = width // GROUP_FEATURES
    weight_rows = jnp.concatenate([out_state, out_conv], axis=0)
    columns = lax.all_to_all(weight_rows, "tp", split_axis=1, concat_axis=0, tiled=True)

    def whole(shape):
        return pl.BlockSpec(shape, lambda i: (0,) * len(shape))

    def rows(n):
        return pl.BlockSpec((ROWS, n), lambda i: (i, 0))

    read, qdev, gate, conv, state, log, tail, head_conv, head_gate = pl.pallas_call(
        local_kernel,
        grid=(count // ROWS,),
        in_specs=[rows(feats), whole((1, feats))] + [whole((feats, width))] * 4
        + [whole((feats, channels))] * 3
        + [whole((1, width)), rows(width), whole((TAPS, channels)), whole((1, GROUP_FEATURES))],
        out_specs=[
            rows(width), rows(width), rows(width), rows(channels),
            whole((heads, GROUP_FEATURES, GROUP_FEATURES)), whole((1, width)),
            whole((HALO, channels)), whole((HALO, channels)), whole((HALO, channels)),
        ],
        out_shape=[
            jax.ShapeDtypeStruct((count, width), f32),
            jax.ShapeDtypeStruct((count, width), bf16),
            jax.ShapeDtypeStruct((count, width), bf16),
            jax.ShapeDtypeStruct((count, channels), bf16),
            jax.ShapeDtypeStruct((heads, GROUP_FEATURES, GROUP_FEATURES), bf16),
            jax.ShapeDtypeStruct((1, width), f32),
            jax.ShapeDtypeStruct((HALO, channels), bf16),
            jax.ShapeDtypeStruct((HALO, channels), bf16),
            jax.ShapeDtypeStruct((HALO, channels), bf16),
        ],
        scratch_shapes=[
            pltpu.VMEM((HALO + ROWS, channels), f32),
            pltpu.VMEM((heads, GROUP_FEATURES, GROUP_FEATURES), f32),
            pltpu.VMEM((1, width), f32),
        ],
        compiler_params=pltpu.CompilerParams(vmem_limit_bytes=48 * 2**20),
        cost_estimate=pl.CostEstimate(
            flops=2 * count * feats * (4 * width + 3 * channels),
            bytes_accessed=2 * feats * (count + 4 * width + 3 * channels),
            transcendentals=8 * count * width,
        ),
    )(
        tokens, in_gain[None], w_query, w_forget, w_input, w_outgate, w_conv_h, w_conv_b, w_conv_c,
        forget_floor[None], forget_leak, conv_taps, group_gain[None],
    )
    size = lax.axis_size("sp")
    rim = lax.ppermute(tail, "sp", [(i, i + 1) for i in range(size - 1)])
    states = lax.all_gather(state, "sp")
    logs = lax.all_gather(log, "sp")
    mixed = pl.pallas_call(
        merge_kernel,
        grid=(count // ROWS,),
        in_specs=[
            rows(width), rows(width), rows(width), rows(channels), whole(states.shape), whole(logs.shape),
            whole(rim.shape), whole(rim.shape), whole(rim.shape),
            whole((1, GROUP_FEATURES)), whole((1, GROUP_FEATURES)), whole((TAPS, channels)),
        ],
        out_specs=rows(width + channels),
        out_shape=jax.ShapeDtypeStruct((count, width + channels), bf16),
        scratch_shapes=[pltpu.VMEM((heads, GROUP_FEATURES, GROUP_FEATURES), f32)],
        compiler_params=pltpu.CompilerParams(vmem_limit_bytes=32 * 2**20),
    )(
        read, qdev, gate, conv, states, logs, rim, head_conv, head_gate,
        state_gain[None], group_gain[None], conv_taps,
    )
    everything = lax.all_gather(mixed, "tp", axis=1, tiled=True)
    return jnp.dot(everything, columns, preferred_element_type=f32).astype(bf16)


def solution(mesh):
    cols, rows = P(None, "tp"), P("tp", None)
    in_specs = (
        P("sp", None), P(), cols, cols, cols, cols, cols, cols, cols,
        P("tp"), P("sp", "tp"), P(), cols, P(), rows, rows,
    )
    return jax.shard_map(
        body, mesh=mesh, in_specs=in_specs, out_specs=P("sp", "tp"), check_vma=False
    )
```

```python
import functools

import jax
import jax.numpy as jnp
from jax import lax
from jax.experimental import pallas as pl
from jax.experimental.pallas import tpu as pltpu
from jax.sharding import PartitionSpec as P

GROUP_FEATURES = 128
CHUNK = 128
ROWS = 256
TAPS = 3
HALO = 8

norm_eps = 1e-06
f32 = jnp.float32
bf16 = jnp.bfloat16


def dot(a, b, dims=((1,), (0,)), precision=None):
    return lax.dot_general(a, b, (dims, ((), ())), precision=precision, preferred_element_type=f32)


def rms(values):
    return values * lax.rsqrt(jnp.mean(values * values, axis=-1, keepdims=True) + norm_eps)


def per_group(values, gain):
    parts = []
    for g in range(values.shape[1] // GROUP_FEATURES):
        parts.append(rms(values[:, g * GROUP_FEATURES : (g + 1) * GROUP_FEATURES]) * gain)
    return jnp.concatenate(parts, axis=1)


def fused_kernel(
    tp, sp,
    tokens, in_gain, wq, wf, wi, wg, wh, wb, wc, floor, leak, state_gain, taps, group_gain,
    out_state, out_conv, result,
    pad, state, offset, read, qdev, gate, conv_all, mix_all, columns, states, logs, sent_state,
    rim, tail, head_conv, head_gate, incoming,
    col_send, col_recv, own_sem, blk_send, fwd_send, blk_recv, st_send, st_recv, log_send, log_recv,
    rim_send, rim_recv,
):
    step, steps = pl.program_id(0), pl.num_programs(0)
    rows = tokens.shape[0]
    me, place = lax.axis_index("tp"), lax.axis_index("sp")
    partner = me + 1 - 2 * lax.rem(me, 2)
    ncols = result.shape[1]
    heads = state.shape[0]
    here = pl.ds(pl.multiple_of(step * rows, rows), rows)
    held = (conv_all, mix_all)

    def col_copy(kind, k):
        target = lax.rem(me + k, tp)
        src = (out_state, out_conv)[kind].at[:, pl.ds(pl.multiple_of(target * ncols, ncols), ncols)]
        dst = columns.at[kind, me]
        if k == 0:
            return pltpu.make_async_copy(src, dst, own_sem.at[kind])
        return pltpu.make_async_remote_copy(
            src, dst, col_send.at[kind, k], col_recv.at[kind, me], device_id={"tp": target}
        )

    def block_copy(kind, t, origin, target, send):
        ref = held[kind].at[origin, t]
        return pltpu.make_async_remote_copy(
            ref, ref, send, blk_recv.at[kind, origin, t], device_id={"tp": target}
        )

    def own_copies(kind, t):
        out = [block_copy(kind, t, me, partner, blk_send.at[kind, 0, t])]
        for k in range(1, tp // 2):
            out.append(block_copy(kind, t, me, lax.rem(me + 2 * k, tp), blk_send.at[kind, k, t]))
        return out

    def relays(kind, t):
        out = []
        for k in range(1, tp // 2):
            origin = lax.rem(me + 2 * k, tp)
            out.append(block_copy(kind, t, origin, partner, fwd_send.at[kind, k, t]))
        return out

    def state_copies(k):
        target = lax.rem(place + k, sp)
        to = {"sp": target}
        return (
            pltpu.make_async_remote_copy(
                sent_state, states.at[place], st_send.at[k], st_recv.at[place], device_id=to
            ),
            pltpu.make_async_remote_copy(
                offset, logs.at[place], log_send.at[k], log_recv.at[place], device_id=to
            ),
        )

    def state_arrivals(k):
        source = lax.rem(place + k, sp)
        to = {"sp": source}
        return (
            pltpu.make_async_remote_copy(
                sent_state, states.at[source], st_send.at[k], st_recv.at[source], device_id=to
            ),
            pltpu.make_async_remote_copy(
                offset, logs.at[source], log_send.at[k], log_recv.at[source], device_id=to
            ),
        )

    rim_copy = pltpu.make_async_remote_copy(
        tail, rim, rim_send.at[0], rim_recv.at[0], device_id={"sp": lax.rem(place + 1, sp)}
    )

    @pl.when(step == 0)
    def _():
        barrier = pltpu.get_barrier_semaphore()
        for k in range(1, tp):
            pl.semaphore_signal(barrier, inc=1, device_id={"tp": lax.rem(me + k, tp)})
        for k in range(1, sp):
            pl.semaphore_signal(barrier, inc=1, device_id={"sp": lax.rem(place + k, sp)})
        pl.semaphore_wait(barrier, tp + sp - 2)
        for kind in (1, 0):
            for k in range(tp):
                col_copy(kind, k).start()
        pad[0:HALO, :] = jnp.zeros((HALO, pad.shape[1]), f32)
        state[...] = jnp.zeros_like(state)
        offset[...] = jnp.zeros_like(offset)

    normed = (rms(tokens[...].astype(f32)) * in_gain[...]).astype(bf16)

    def project(w):
        return dot(normed, w[...]).astype(bf16).astype(f32)

    conv_in = (project(wc) * project(wh)).astype(bf16).astype(f32)
    proj_b = project(wb)
    pad[HALO : HALO + rows, :] = conv_in
    w = taps[...].astype(f32)
    total = w[TAPS - 1 : TAPS] * conv_in
    for j in range(TAPS - 1):
        total += w[j : j + 1] * pad[HALO - (TAPS - 1) + j : HALO - (TAPS - 1) + j + rows, :]
    conv_all[me, step] = per_group(proj_b * total, group_gain[...]).astype(bf16)

    @pl.when(step == 0)
    def _():
        head_conv[...] = conv_in[:HALO]
        head_gate[...] = proj_b[:HALO]

    pad[0:HALO, :] = conv_in[rows - HALO :]

    x = project(wf)
    key = (1.0 - floor[...]) * jax.nn.sigmoid(-x)
    logf = jnp.log(1.0 - key) + leak[...]
    value = dot(normed, wi[...]).astype(bf16)
    query = jax.nn.silu(project(wq))
    gate[here, :] = dot(normed, wg[...]).astype(bf16)

    r = lax.broadcasted_iota(jnp.int32, (CHUNK, CHUNK), 0)
    c = lax.broadcasted_iota(jnp.int32, (CHUNK, CHUNK), 1)
    causal = r >= c
    ones = causal.astype(f32)
    for b in range(rows // CHUNK):
        lo, hi = b * CHUNK, (b + 1) * CHUNK
        at = pl.ds(pl.multiple_of(step * rows + lo, CHUNK), CHUNK)
        cum = dot(ones, logf[lo:hi], precision=lax.Precision.HIGHEST)
        mid = cum[CHUNK // 2 - 1 : CHUNK // 2]
        last = cum[CHUNK - 1 : CHUNK]
        q_mid = query[lo:hi] * jnp.exp(cum - mid)
        k_mid = key[lo:hi] * jnp.exp(mid - cum)
        q_all = q_mid * jnp.exp(mid)
        k_end = (k_mid * jnp.exp(last - mid)).astype(bf16)
        qdev[at, :] = (q_all * jnp.exp(offset[0:1, :])).astype(bf16)
        q_mid, k_mid, q_all = q_mid.astype(bf16), k_mid.astype(bf16), q_all.astype(bf16)
        for h in range(heads):
            s = slice(h * GROUP_FEATURES, (h + 1) * GROUP_FEATURES)
            scores = dot(q_mid[:, s], k_mid[:, s], ((1,), (1,)))
            scores = jnp.where(causal, scores, 0.0).astype(bf16)
            v = value[lo:hi, s]
            old = state[h]
            read[at, s] = dot(scores, v) + dot(q_all[:, s], old.astype(bf16), ((1,), (1,)))
            state[h] = old * jnp.exp(last[:, s]) + dot(v, k_end[:, s], ((0,), (0,)))
        offset[...] += last

    @pl.when(step > 0)
    def _():
        for copy in own_copies(0, step):
            copy.start()

    @pl.when(step == steps - 1)
    def _():
        nb = read.shape[0] // rows
        tail[...] = pad[0:HALO, :]
        sent_state[...] = state[...].astype(bf16)
        rim_copy.start()
        for k in range(1, sp):
            for copy in state_copies(k):
                copy.start()
        rim_copy.wait_recv()
        before = jnp.where(place > 0, rim[...], 0.0)
        ext = jnp.concatenate([before, head_conv[...]], axis=0)
        fixed = w[TAPS - 1 : TAPS] * head_conv[...]
        for j in range(TAPS - 1):
            fixed += w[j : j + 1] * ext[HALO - (TAPS - 1) + j : 2 * HALO - (TAPS - 1) + j]
        fixed = per_group(head_gate[...] * fixed, group_gain[...])
        conv_all[me, 0, 0:HALO, :] = fixed.astype(bf16)

        for k in range(1, sp):
            for copy in state_arrivals(k):
                copy.wait_recv()
        for copy in own_copies(0, 0):
            copy.start()
        incoming[...] = jnp.zeros_like(incoming)

        def hop(p, _):
            decay = jnp.exp(logs[p, 0:1, :])
            for h in range(heads):
                s = slice(h * GROUP_FEATURES, (h + 1) * GROUP_FEATURES)
                incoming[h] = incoming[h] * decay[:, s] + states[p, h].astype(f32)
            return 0

        lax.fori_loop(0, place, hop, 0)

        def merge(t, _):
            at = pl.ds(pl.multiple_of(t * rows, rows), rows)
            for h in range(heads):
                s = slice(h * GROUP_FEATURES, (h + 1) * GROUP_FEATURES)
                whole = read[at, s] + dot(qdev[at, s], incoming[h].astype(bf16), ((1,), (1,)))
                out = rms(whole) * state_gain[...] * jax.nn.silu(gate[at, s].astype(f32))
                mix_all[me, t, :, s] = out.astype(bf16)
            for copy in own_copies(1, t):
                copy.start()
            return 0

        lax.fori_loop(0, nb, merge, 0)

        def relay(kind, t):
            for copy in relays(kind, t):
                copy.wait_recv()
                copy.start()

        def conv_relay(t, _):
            relay(0, t + 1)
            return 0

        lax.fori_loop(0, nb - 1, conv_relay, 0)
        relay(0, 0)
        for kind in range(2):
            col_copy(kind, 0).wait()
            for k in range(1, tp):
                source = lax.rem(me + k, tp)
                ref = columns.at[kind, source]
                pltpu.make_async_remote_copy(
                    ref, ref, col_send.at[kind, k], col_recv.at[kind, source],
                    device_id={"tp": source},
                ).wait_recv()

        def finish(t, _):
            relay(1, t)
            for kind in range(2):
                for k in range(tp // 2):
                    origin = lax.rem(partner + 2 * k, tp)
                    block_copy(kind, t, origin, partner, blk_send.at[kind, 0, t]).wait_recv()
            acc = jnp.zeros((rows, ncols), f32)
            for o in range(tp):
                acc += dot(mix_all[o, t], columns[0, o])
                acc += dot(conv_all[o, t], columns[1, o])
            result[pl.ds(pl.multiple_of(t * rows, rows), rows), :] = acc.astype(bf16)
            return 0

        lax.fori_loop(0, nb, finish, 0)

        def drain(t, _):
            for kind in range(2):
                for copy in own_copies(kind, t) + relays(kind, t):
                    copy.wait_send()
            return 0

        lax.fori_loop(0, nb, drain, 0)
        for kind in range(2):
            for k in range(1, tp):
                col_copy(kind, k).wait_send()
        rim_copy.wait_send()
        for k in range(1, sp):
            for copy in state_copies(k):
                copy.wait_send()


def body(
    tokens, in_gain, w_query, w_forget, w_input, w_outgate, w_conv_h, w_conv_b, w_conv_c,
    forget_floor, forget_leak, state_gain, conv_taps, group_gain, out_state, out_conv,
):
    count, feats = tokens.shape
    width, channels = w_query.shape[1], w_conv_h.shape[1]
    heads = width // GROUP_FEATURES
    tp, sp = lax.axis_size("tp"), lax.axis_size("sp")
    ncols, nb = out_state.shape[1] // tp, count // ROWS

    def whole(*shape):
        return pl.BlockSpec(shape, lambda i: (0,) * len(shape))

    def rows(n):
        return pl.BlockSpec((ROWS, n), lambda i: (i, 0))

    sems = pltpu.SemaphoreType.DMA
    return pl.pallas_call(
        functools.partial(fused_kernel, tp, sp),
        grid=(nb,),
        in_specs=[rows(feats), whole(1, feats)] + [whole(feats, width)] * 4
        + [whole(feats, channels)] * 3
        + [whole(1, width), rows(width), whole(1, GROUP_FEATURES), whole(TAPS, channels),
           whole(1, GROUP_FEATURES)]
        + [pl.BlockSpec(memory_space=pl.ANY)] * 2,
        out_specs=whole(count, ncols),
        out_shape=jax.ShapeDtypeStruct((count, ncols), bf16),
        scratch_shapes=[
            pltpu.VMEM((HALO + ROWS, channels), f32),
            pltpu.VMEM((heads, GROUP_FEATURES, GROUP_FEATURES), f32),
            pltpu.VMEM((HALO, width), f32),
            pltpu.VMEM((count, width), f32),
            pltpu.VMEM((count, width), bf16),
            pltpu.VMEM((count, width), bf16),
            pltpu.VMEM((tp, nb, ROWS, channels), bf16),
            pltpu.VMEM((tp, nb, ROWS, width), bf16),
            pltpu.VMEM((2, tp, width, ncols), bf16),
            pltpu.VMEM((sp, heads, GROUP_FEATURES, GROUP_FEATURES), bf16),
            pltpu.VMEM((sp, HALO, width), f32),
            pltpu.VMEM((heads, GROUP_FEATURES, GROUP_FEATURES), bf16),
            pltpu.VMEM((HALO, channels), f32),
            pltpu.VMEM((HALO, channels), f32),
            pltpu.VMEM((HALO, channels), f32),
            pltpu.VMEM((HALO, channels), f32),
            pltpu.VMEM((heads, GROUP_FEATURES, GROUP_FEATURES), f32),
            sems((2, tp)), sems((2, tp)), sems((2,)),
            sems((2, tp // 2, nb)), sems((2, tp // 2, nb)), sems((2, tp, nb)),
            sems((sp,)), sems((sp,)), sems((sp,)), sems((sp,)), sems((1,)), sems((1,)),
        ],
        compiler_params=pltpu.CompilerParams(
            vmem_limit_bytes=56 * 2**20, collective_id=0, has_side_effects=True
        ),
    )(
        tokens, in_gain[None], w_query, w_forget, w_input, w_outgate, w_conv_h, w_conv_b, w_conv_c,
        forget_floor[None], forget_leak, state_gain[None], conv_taps, group_gain[None],
        out_state, out_conv,
    )


def solution(mesh):
    cols, rows = P(None, "tp"), P("tp", None)
    in_specs = (
        P("sp", None), P(), cols, cols, cols, cols, cols, cols, cols,
        P("tp"), P("sp", "tp"), P(), cols, P(), rows, rows,
    )
    return jax.shard_map(
        body, mesh=mesh, in_specs=in_specs, out_specs=P("sp", "tp"), check_vma=False
    )
```
